32 devices in a mesh: sp: 4 (over y, x), tp: 8 (over z, core).
Axes of the slice: x: 2, y: 2, z: 4, core: 2. Of those that a mesh axis runs over, the one named last changes fastest.
Arguments:
- conv_value: bfloat16 [6144, 2048], P('sp', 'tp'), may hold values from -48 to 48
- conv_gate: bfloat16 [6144, 2048], P('sp', 'tp'), may hold values from -6 to 6
- doc_ids: int32 [6144], P('sp'), may hold values from 0 to 3, never falling along the last dimension, each value on 1 to 4608 neighbouring positions
- conv_kernel: bfloat16 [31, 2048], P(None, 'tp'), may hold values from -1 to 1
- norm_gain_conv: float32 [2048], replicated, may hold values from 0.1 to 1.9
- norm_bias_conv: float32 [2048], replicated, may hold values from -3 to 3
- proj_weight: bfloat16 [2048, 2048], P('tp'), may hold values from -0.125 to 0.125
- residual: bfloat16 [6144, 2048], P(('sp', 'tp')), may hold values from -6 to 6
- norm_gain_moe: float32 [2048], replicated, may hold values from 0.1 to 1.9
- group_router: bfloat16 [2048, 2], replicated, may hold values from -0.125 to 0.125
- expert_router: bfloat16 [2048, 4], replicated, may hold values from -0.125 to 0.125
- routing: int32 [6144, 2], P(('sp', 'tp')), may hold values from 0 to 3, as said below
- expert_gate_w: bfloat16 [4, 2048, 512], P('sp'), may hold values from -0.125 to 0.125
- expert_up_w: bfloat16 [4, 2048, 512], P('sp'), may hold values from -0.125 to 0.125
- expert_down_w: bfloat16 [4, 512, 2048], P('sp'), may hold values from -0.25 to 0.25
Outputs:
- output: bfloat16 [6144, 2048], P(('sp', 'tp'))
The draws below stay inside these ranges and needn't reach their ends.
Inputs may be any that keep to these rules, and one draw needn't show every extreme that they name: `routing`: both numbers of a row are different experts of one group (expert // 2); within the rows of one device (aligned blocks of 192 rows) every expert is named exactly 96 times.
All inputs are finite; a program needn't handle non-finite values.
Results may differ from the reference program's by a relative error of at most 0.015.
Values may be sent and summed in bfloat16 or wider, within the bound.
A program may use at most 64 MiB of HBM per device.

```python
import math
import jax
import jax.numpy as jnp
import numpy as np
from jax import lax

D = 2048
CH = 2048
KW = 31
FF = 512
GROUPS = 2
TOK_DEV = 192
EXPERTS = 4
TOKENS = 6144
DOCS = 4
DOC_MOST = 4608


def draw_conv_value(key, part):
    base_key = jax.random.fold_in(key, 101)
    column_key = jax.random.fold_in(key, 102)
    column_scale = 3.0 ** (jnp.arange(CH, dtype=jnp.float32) / CH) * jax.random.uniform(column_key, (CH,), jnp.float32, 0.6, 1.6)
    base = jnp.clip(jax.random.normal(base_key, (TOKENS, CH), jnp.float32), -6.0, 6.0)
    return (base * column_scale[None, :]).astype(jnp.bfloat16)


def draw_routing(key, part):
    blocks = TOKENS // TOK_DEV
    per_group = EXPERTS // GROUPS
    group_rows = TOK_DEV // GROUPS
    per_expert = TOK_DEV // EXPERTS
    shift_key = jax.random.fold_in(key, 201)
    flip_key = jax.random.fold_in(key, 202)
    shuffle_key = jax.random.fold_in(key, 203)
    rank_order = jnp.arange(TOK_DEV, dtype=jnp.int32)
    first_local = rank_order % group_rows // per_expert
    shifts = jax.random.randint(shift_key, (blocks,), 1, per_group, jnp.int32)
    flips = jax.random.randint(flip_key, (blocks,), 0, GROUPS, jnp.int32)
    group_index = (rank_order[None, :] // group_rows + flips[:, None]) % GROUPS
    second_local = (first_local[None, :] + shifts[:, None]) % per_group
    first_expert = group_index * per_group + first_local[None, :]
    second_expert = group_index * per_group + second_local
    pairing = jnp.stack([first_expert, second_expert], axis=-1).astype(jnp.int32)
    shuffles = jax.vmap(lambda block_key: jax.random.permutation(block_key, TOK_DEV))(jax.random.split(shuffle_key, blocks))

    def place_block(shuffle, block_pairs):
        return jnp.zeros((TOK_DEV, 2), jnp.int32).at[shuffle].set(block_pairs)
    routed = jax.vmap(place_block)(shuffles.astype(jnp.int32), pairing)
    return routed.reshape(TOKENS, 2).astype(jnp.int32)


def shard_levels(key, dims, cuts, smallest, high):
    loudness, own = 1.0, jax.random.fold_in(key, 6)
    for axis_at, shards_of in cuts:
        steps = jnp.exp(jax.random.uniform(jax.random.fold_in(own, axis_at), (shards_of,), jnp.float32, smallest / len(cuts), high / len(cuts)))
        loudness = loudness * jnp.repeat(steps, dims[axis_at] // shards_of).reshape([-1 if axis == axis_at else 1 for axis in range(len(dims))])
    return loudness


def length_profile(count, total, reach, lean):
    portions = [(1 << 20) // math.isqrt(grade ** lean) + 1 for grade in range(2, count + 1)]
    surplus, given = total - reach - (count - 1), [1] * (count - 1)
    while surplus > 0:
        movable = [i for i in range(count - 1) if given[i] < reach]
        mass, budget = sum([portions[i] for i in movable]), surplus
        for i in movable:
            more = min(reach - given[i], max(1, budget * portions[i] // mass), surplus)
            given[i] = given[i] + more
            surplus = surplus - more
    return np.array([reach] + given)


def ragged_sizes(rng, number_of, total, limit, skew):
    if number_of == 2:
        one = jax.random.randint(rng, (), max(1, total - limit), min(limit, total - 1) + 1)
        return jnp.stack([one, total - one])
    tallies = jnp.asarray(length_profile(number_of, total, limit, skew), jnp.int32)
    couples = (number_of - 1) // 2
    donor, taker = tallies[1:1 + 2 * couples:2], tallies[2:2 + 2 * couples:2]
    room = jnp.minimum(donor - 1, limit - taker)
    moved = jax.random.randint(jax.random.fold_in(rng, 1), (couples,), 0, 1 << 20) % (room + 1)
    tallies = tallies.at[1:1 + 2 * couples:2].set(donor - moved).at[2:2 + 2 * couples:2].set(taker + moved)
    return tallies[jax.random.permutation(jax.random.fold_in(rng, 2), number_of)]


def normal_values(key, extent, spread, limit, cuts=(), kind=jnp.bfloat16):
    array = jax.random.normal(key, extent, jnp.float32) * spread
    if len(cuts) > 0:
        array = shard_levels(key, extent, cuts, -0.22, 0.18) * array
    return jnp.clip(array, min=-limit, max=limit).astype(kind)


def setup_inputs(seed: int = 0) -> dict:
    seeds = jax.random.split(jax.random.key(seed), 16)
    return {
        "conv_value": draw_conv_value(jax.random.fold_in(seeds[15], 71), 0),
        "conv_gate": normal_values(seeds[1], (TOKENS, CH), 1.0, 6.0, ((0, 4), (1, 8))),
        "doc_ids": jnp.searchsorted(jnp.cumsum(ragged_sizes(seeds[2], DOCS, TOKENS, DOC_MOST, 0)), jnp.arange(TOKENS), side="right").astype(jnp.int32),
        "conv_kernel": normal_values(seeds[3], (KW, CH), KW ** -0.5, 1.0, ((1, 8),)),
        "norm_gain_conv": jnp.clip(1.0 + 0.18 * jax.random.normal(seeds[4], (CH,), jnp.float32), 0.1, 1.9),
        "norm_bias_conv": normal_values(seeds[5], (CH,), 0.5, 3.0, (), jnp.float32),
        "proj_weight": normal_values(seeds[6], (CH, D), CH ** -0.5, 0.125, ((0, 8),)),
        "residual": normal_values(seeds[7], (TOKENS, D), 1.0, 6.0, ((0, 32),)),
        "norm_gain_moe": jnp.clip(1.0 + 0.18 * jax.random.normal(seeds[8], (D,), jnp.float32), 0.1, 1.9),
        "group_router": normal_values(seeds[9], (D, GROUPS), D ** -0.5, 0.125),
        "expert_router": normal_values(seeds[10], (D, EXPERTS), D ** -0.5, 0.125),
        "routing": draw_routing(jax.random.fold_in(seeds[15], 71), 0),
        "expert_gate_w": normal_values(seeds[12], (EXPERTS, D, FF), D ** -0.5, 0.125, ((0, 4),)),
        "expert_up_w": normal_values(seeds[13], (EXPERTS, D, FF), D ** -0.5, 0.125, ((0, 4),)),
        "expert_down_w": normal_values(seeds[14], (EXPERTS, FF, D), FF ** -0.5, 0.25, ((0, 4),)),
    }


epsilon = 1e-06

def reference(conv_value, conv_gate, doc_ids, conv_kernel, norm_gain_conv, norm_bias_conv, proj_weight, residual, norm_gain_moe, group_router, expert_router, routing, expert_gate_w, expert_up_w, expert_down_w):
    gated_values = (conv_value.astype(jnp.float32) * jax.nn.sigmoid(conv_gate.astype(jnp.float32))).astype(jnp.bfloat16)
    rim_width = KW - 1
    length = gated_values.shape[0]
    padded = jnp.concatenate([jnp.zeros((rim_width, CH), jnp.bfloat16), gated_values], axis=0)
    padded_ids = jnp.concatenate([jnp.zeros((rim_width,), jnp.int32), doc_ids.astype(jnp.int32)], axis=0)
    kernel = conv_kernel.astype(jnp.float32)
    summed = jnp.zeros((length, CH), jnp.float32)
    for tap in range(KW):
        same_doc = padded_ids[tap:tap + length] == doc_ids
        summed = summed + jnp.where(same_doc[:, None], padded[tap:tap + length].astype(jnp.float32) * kernel[tap][None, :], jnp.float32(0.0))
    convolved = summed.astype(jnp.bfloat16)
    values = convolved.astype(jnp.float32)
    average = lax.optimization_barrier(jnp.mean(values, axis=1, keepdims=True))
    centered = values - average
    variance = lax.optimization_barrier(jnp.mean(centered * centered, axis=1, keepdims=True))
    activated = jax.nn.silu(centered * lax.rsqrt(variance + epsilon) * norm_gain_conv + norm_bias_conv).astype(jnp.bfloat16)
    projected = jnp.dot(activated, proj_weight, preferred_element_type=jnp.float32)
    hidden_state = (residual.astype(jnp.float32) + projected).astype(jnp.bfloat16)
    state_values = hidden_state.astype(jnp.float32)
    normed = (state_values * lax.rsqrt(lax.optimization_barrier(jnp.mean(state_values * state_values, axis=1, keepdims=True)) + epsilon) * norm_gain_moe).astype(jnp.bfloat16)
    group_logits = jnp.dot(normed, group_router, preferred_element_type=jnp.float32)
    expert_logits = jnp.dot(normed, expert_router, preferred_element_type=jnp.float32)
    per_group = EXPERTS // GROUPS
    chosen_group = (routing[:, 0] // per_group).astype(jnp.int32)
    group_exp = jnp.exp(group_logits)
    group_prob = jnp.take_along_axis(group_exp, chosen_group[:, None], axis=1)[:, 0] / lax.optimization_barrier(jnp.sum(group_exp, axis=1))
    first_logit = jnp.take_along_axis(expert_logits, routing[:, 0:1], axis=1)[:, 0]
    second_logit = jnp.take_along_axis(expert_logits, routing[:, 1:2], axis=1)[:, 0]
    first_exp = jnp.exp(first_logit)
    second_exp = jnp.exp(second_logit)
    first_weight = group_prob * first_exp / (first_exp + second_exp)
    second_weight = group_prob * second_exp / (first_exp + second_exp)
    per_expert = 2 * length // EXPERTS
    flat_experts = routing.reshape(-1).astype(jnp.int32)
    ordering = jnp.argsort(flat_experts, stable=True).astype(jnp.int32)
    slot_table = ordering.reshape(EXPERTS, per_expert)

    def one_expert(operands):
        assigned, gate_matrix, up_matrix, down_matrix = operands
        token_rows = normed[assigned // 2]
        gate_part = jnp.dot(token_rows, gate_matrix, preferred_element_type=jnp.float32)
        up_part = jnp.dot(token_rows, up_matrix, preferred_element_type=jnp.float32)
        expert_hidden = (jax.nn.silu(gate_part) * up_part).astype(jnp.bfloat16)
        return jnp.dot(expert_hidden, down_matrix, preferred_element_type=jnp.float32).astype(jnp.bfloat16)
    results = lax.map(one_expert, (slot_table, expert_gate_w, expert_up_w, expert_down_w))
    per_assignment = jnp.zeros((2 * length, D), jnp.bfloat16).at[slot_table.reshape(-1)].set(results.reshape(-1, D))
    picked = per_assignment.reshape(length, 2, D).astype(jnp.float32)
    mixture = first_weight[:, None] * picked[:, 0] + second_weight[:, None] * picked[:, 1]
    return (state_values + mixture).astype(jnp.bfloat16)
```

```python
import jax
import jax.numpy as jnp
from jax import lax
from jax.sharding import PartitionSpec as P

epsilon = 1e-06


def halo(gated_values, doc_ids, rim_width):
    local_tokens, local_width = gated_values.shape
    last_id = doc_ids[local_tokens - 1]
    same = doc_ids[local_tokens - rim_width :] == last_id
    rim = jnp.where(same[:, None], gated_values[local_tokens - rim_width :], jnp.bfloat16(0.0))
    id_row = jnp.full((1, local_width), last_id.astype(jnp.bfloat16))
    count = lax.axis_size("sp")
    pairs = [(i, i + 1) for i in range(count - 1)]
    return lax.ppermute(jnp.concatenate([rim, id_row], axis=0), "sp", pairs)


def body(
    conv_value,
    conv_gate,
    doc_ids,
    conv_kernel,
    norm_gain_conv,
    norm_bias_conv,
    proj_weight,
    residual,
    norm_gain_moe,
    group_router,
    expert_router,
    routing,
    expert_gate_w,
    expert_up_w,
    expert_down_w,
):
    local_tokens, local_width = conv_value.shape
    kernel_taps = conv_kernel.shape[0]
    rim_width = kernel_taps - 1
    sp_size = lax.axis_size("sp")
    tp_size = lax.axis_size("tp")
    weight_rows = proj_weight.shape[0] // sp_size
    weight_piece = lax.dynamic_slice_in_dim(
        proj_weight, lax.axis_index("sp") * weight_rows, weight_rows
    )
    weight_full = lax.all_gather(weight_piece, ("sp", "tp"), axis=0, tiled=True)
    gated_values = (
        conv_value.astype(jnp.float32) * jax.nn.sigmoid(conv_gate.astype(jnp.float32))
    ).astype(jnp.bfloat16)
    arrived_rim = halo(gated_values, doc_ids, rim_width)
    rim_id = arrived_rim[rim_width, 0].astype(jnp.int32)
    padded = jnp.concatenate([arrived_rim[:rim_width], gated_values], axis=0)
    padded_ids = jnp.concatenate([jnp.full((rim_width,), rim_id), doc_ids], axis=0)
    kernel = conv_kernel.astype(jnp.float32)
    summed = jnp.zeros((local_tokens, local_width), jnp.float32)
    for tap in range(kernel_taps):
        same_doc = padded_ids[tap : tap + local_tokens] == doc_ids
        summed = summed + jnp.where(
            same_doc[:, None],
            padded[tap : tap + local_tokens].astype(jnp.float32) * kernel[tap][None, :],
            jnp.float32(0.0),
        )
    convolved = summed.astype(jnp.bfloat16)
    values = lax.all_to_all(convolved, "tp", split_axis=0, concat_axis=1, tiled=True).astype(
        jnp.float32
    )
    average = jnp.mean(values, axis=1, keepdims=True)
    centered = values - average
    variance = jnp.mean(centered * centered, axis=1, keepdims=True)
    activated = jax.nn.silu(
        centered * lax.rsqrt(variance + epsilon) * norm_gain_conv + norm_bias_conv
    ).astype(jnp.bfloat16)
    rows, channels = activated.shape
    reordered = (
        activated.reshape(rows, tp_size, sp_size, weight_rows)
        .transpose(0, 2, 1, 3)
        .reshape(rows, channels)
    )
    projected = jnp.dot(reordered, weight_full, preferred_element_type=jnp.float32)
    hidden_state = (residual.astype(jnp.float32) + projected).astype(jnp.bfloat16)
    state_values = hidden_state.astype(jnp.float32)
    normed = (
        state_values
        * lax.rsqrt(jnp.mean(state_values * state_values, axis=1, keepdims=True) + epsilon)
        * norm_gain_moe
    ).astype(jnp.bfloat16)
    group_total = group_router.shape[1]
    expert_total = expert_router.shape[1]
    per_group = expert_total // group_total
    capacity = 2 * rows // expert_total
    expert_iota = jnp.arange(expert_total, dtype=jnp.int32)[None, :]
    chosen = (routing[:, 0:1] == expert_iota) | (routing[:, 1:2] == expert_iota)
    chosen_group = (routing[:, 0:1] // per_group) == jnp.arange(group_total, dtype=jnp.int32)[
        None, :
    ]
    row_iota = jnp.arange(rows, dtype=jnp.int32)
    earlier = (row_iota[None, :] < row_iota[:, None]).astype(jnp.bfloat16)
    before = jnp.dot(earlier, chosen.astype(jnp.bfloat16), preferred_element_type=jnp.float32)
    slot = jnp.where(chosen, before, jnp.float32(-1.0))
    slot_iota = jnp.arange(capacity, dtype=jnp.int32).astype(jnp.float32)
    picks = (slot.T[:, None, :] == slot_iota[None, :, None]).astype(jnp.bfloat16)
    outgoing = (
        jnp.dot(
            picks.reshape(expert_total * capacity, rows),
            normed,
            preferred_element_type=jnp.float32,
        )
        .astype(jnp.bfloat16)
        .reshape(sp_size, -1, capacity, channels)
    )
    arrived = lax.all_to_all(outgoing, "sp", split_axis=0, concat_axis=0, tiled=True)
    group_logits = jnp.dot(normed, group_router, preferred_element_type=jnp.float32)
    expert_logits = jnp.dot(normed, expert_router, preferred_element_type=jnp.float32)
    group_exp = jnp.exp(group_logits)
    group_prob = jnp.sum(
        jnp.where(chosen_group, group_exp, jnp.float32(0.0)), axis=1, keepdims=True
    ) / jnp.sum(group_exp, axis=1, keepdims=True)
    chosen_exp = jnp.where(chosen, jnp.exp(expert_logits), jnp.float32(0.0))
    mix_weight = group_prob * chosen_exp / jnp.sum(chosen_exp, axis=1, keepdims=True)
    flattened = arrived.reshape(-1, channels)
    gate_part = jnp.dot(flattened, expert_gate_w[0], preferred_element_type=jnp.float32)
    up_part = jnp.dot(flattened, expert_up_w[0], preferred_element_type=jnp.float32)
    expert_hidden = (jax.nn.silu(gate_part) * up_part).astype(jnp.bfloat16)
    expert_result = jnp.dot(
        expert_hidden, expert_down_w[0], preferred_element_type=jnp.float32
    ).astype(jnp.bfloat16)
    returned = lax.all_to_all(
        expert_result.reshape(sp_size, -1, channels),
        "sp",
        split_axis=0,
        concat_axis=0,
        tiled=True,
    ).reshape(expert_total * capacity, channels)
    spread = jnp.where(
        slot[:, :, None] == slot_iota[None, None, :], mix_weight[:, :, None], jnp.float32(0.0)
    )
    mixture = jnp.dot(
        spread.astype(jnp.bfloat16).reshape(rows, expert_total * capacity),
        returned,
        preferred_element_type=jnp.float32,
    )
    return (state_values + mixture).astype(jnp.bfloat16)


def solution(mesh):
    placed = (
        P("sp", "tp"),
        P("sp", "tp"),
        P("sp"),
        P(None, "tp"),
        P(),
        P(),
        P("tp", None),
        P(("sp", "tp"), None),
        P(),
        P(),
        P(),
        P(("sp", "tp"), None),
        P("sp", None, None),
        P("sp", None, None),
        P("sp", None, None),
    )
    return jax.shard_map(
        body, mesh=mesh, in_specs=placed, out_specs=P(("sp", "tp"), None), check_vma=False
    )
```

```python
import functools

import jax
import jax.numpy as jnp
from jax import lax
from jax.experimental import pallas as pl
from jax.experimental.pallas import tpu as pltpu
from jax.sharding import PartitionSpec as P

epsilon = 1e-06
MESH = pl.DeviceIdType.MESH
F32 = jnp.float32
BF16 = jnp.bfloat16
HALO = 32


def gate(value, gate_value):
    return (value.astype(F32) * jax.nn.sigmoid(gate_value.astype(F32))).astype(BF16)


def kernel(
    S,
    T,
    G,
    value_hbm,
    gate_hbm,
    least_tap_ref,
    rim_keep_ref,
    last_id_ref,
    first_id_ref,
    kernel_ref,
    gain_conv_ref,
    bias_conv_ref,
    weight_hbm,
    residual_hbm,
    gain_moe_ref,
    router_ref,
    routing_ref,
    gate_w_hbm,
    up_w_hbm,
    down_w_hbm,
    out_ref,
    value,
    gates,
    wfull,
    residual,
    gate_w,
    up_w,
    down_w,
    rim_out,
    rim_in,
    padded,
    taps,
    conv_out,
    conv_in,
    act,
    hidden,
    normed,
    outgoing,
    arrived,
    ffn_hidden,
    results,
    returned,
    local_sem,
    wl_sem,
    rim_sem,
    wz_send,
    wz_recv,
    wx_send,
    wx_recv,
    wp_send,
    wp_recv,
    a2a_send,
    a2a_recv,
    disp_send,
    disp_recv,
    ret_send,
    ret_recv,
):
    s = lax.axis_index("sp")
    t = lax.axis_index("tp")
    Z = T // 2
    z = t // 2
    core = t % 2
    partner = 2 * z + 1 - core
    tokens, width = value.shape
    block = tokens // T
    n_taps = kernel_ref.shape[0]
    piece = wfull.shape[3]
    D = S * piece

    def remote(src, dst, send, recv, sp_to, tp_to):
        return pltpu.make_async_remote_copy(
            src_ref=src,
            dst_ref=dst,
            send_sem=send,
            recv_sem=recv,
            device_id=(sp_to, tp_to),
            device_id_type=MESH,
        )

    loads = [
        pltpu.make_async_copy(a, b, local_sem.at[i])
        for i, (a, b) in enumerate(
            [
                (value_hbm, value),
                (gate_hbm, gates),
                (residual_hbm, residual),
                (gate_w_hbm, gate_w),
                (up_w_hbm, up_w),
                (down_w_hbm, down_w),
            ]
        )
    ]
    own_w = [
        pltpu.make_async_copy(
            weight_hbm.at[:, pl.ds(j * piece, piece)], wfull.at[t, j], wl_sem.at[j]
        )
        for j in range(S)
    ]
    loads[0].start()
    loads[1].start()
    for c in own_w:
        c.start()
    for c in loads[2:]:
        c.start()

    barrier = pltpu.get_barrier_semaphore()
    for k in range(1, T):
        pl.semaphore_signal(
            barrier, inc=1, device_id=(s, lax.rem(t + k, T)), device_id_type=MESH
        )
    for k in range(1, S):
        pl.semaphore_signal(
            barrier, inc=1, device_id=(lax.rem(s + k, S), t), device_id_type=MESH
        )
    pl.semaphore_wait(barrier, T + S - 2)

    for c in own_w:
        c.wait()
    waits = []
    for k in range(1, Z):
        to = 2 * lax.rem(z + k, Z) + core
        c = remote(wfull.at[t, s], wfull.at[t, s], wz_send.at[k], wz_recv.at[z], s, to)
        c.start()
        waits.append(c)
    c = remote(wfull.at[t], wfull.at[t], wp_send.at[z], wp_recv.at[z], s, partner)
    c.start()
    waits.append(c)

    loads[0].wait()
    loads[1].wait()
    tail = pl.ds(tokens - HALO, HALO)
    rim = gate(value[tail, :], gates[tail, :]).astype(F32) * rim_keep_ref[...]
    rim_out[0:HALO, :] = rim.astype(BF16)
    rim_out[HALO : HALO + 16, :] = last_id_ref[...]
    rim_copy = remote(
        rim_out, rim_in, rim_sem.at[0], rim_sem.at[1], lax.rem(s + 1, S), t
    )
    rim_copy.start()

    def gate_rows(i, _):
        rows = pl.ds(pl.multiple_of(i * 64, 64), 64)
        to_rows = pl.ds(pl.multiple_of(HALO + i * 64, 32), 64)
        padded[to_rows, :] = gate(value[rows, :], gates[rows, :]).astype(F32)
        return 0

    lax.fori_loop(0, tokens // 64, gate_rows, 0)
    taps[0:n_taps, :] = kernel_ref[...].astype(F32)
    rim_copy.wait()
    same = (rim_in[HALO : HALO + 1, :].astype(F32) == first_id_ref[0:1, :]) & (s > 0)
    padded[0:HALO, :] = jnp.where(same, rim_in[0:HALO, :].astype(F32), jnp.float32(0.0))

    step_rows = 32 if block % 32 == 0 else 8
    lanes = min(width, 128)

    def conv_block(owner):
        def conv_rows(i, _):
            base = pl.multiple_of(owner * block + i * step_rows, 8)
            least = least_tap_ref[pl.ds(base, step_rows), :]
            window = padded[pl.ds(base, step_rows + HALO), :]
            total = jnp.zeros((step_rows, width), F32)
            for tap in range(n_taps):
                at = tap + HALO + 1 - n_taps
                valid = least <= tap
                product = window[at : at + step_rows, :] * taps[tap : tap + 1, :]
                parts = [
                    jnp.where(valid, product[:, j : j + lanes], jnp.float32(0.0))
                    for j in range(0, width, lanes)
                ]
                total = total + jnp.concatenate(parts, axis=1)
            conv_out[
                owner, pl.ds(pl.multiple_of(i * step_rows, step_rows), step_rows), :
            ] = total.astype(BF16)
            return 0

        lax.fori_loop(0, block // step_rows, conv_rows, 0)

    def conv_send(k, _):
        owner = lax.rem(t + k, T)
        conv_block(owner)
        remote(
            conv_out.at[owner],
            conv_in.at[t],
            a2a_send.at[owner],
            a2a_recv.at[t],
            s,
            owner,
        ).start()
        return 0

    lax.fori_loop(1, T, conv_send, 0)
    conv_block(t)
    conv_in[t, :, :] = conv_out[t, :, :]

    for k in range(1, Z):
        from_z = lax.rem(z - k + Z, Z)
        row = 2 * from_z + core
        remote(
            wfull.at[row, s], wfull.at[row, s], wz_send.at[k], wz_recv.at[from_z], s, t
        ).wait_recv()
        for j in range(1, S):
            c = remote(
                wfull.at[row, s],
                wfull.at[row, s],
                wx_send.at[j, from_z],
                wx_recv.at[s, from_z],
                lax.rem(s + j, S),
                t,
            )
            c.start()
            waits.append(c)

    rows = block
    E = S
    cap = 2 * rows // E
    lane = lax.broadcasted_iota(jnp.int32, (rows, 128), 1)
    first = routing_ref[:, 0:1]
    second = routing_ref[:, 1:2]
    chosen = (lane == first + G) | (lane == second + G)
    in_group = lane == first // (E // G)
    tri = lax.broadcasted_iota(jnp.int32, (rows, rows), 0) > lax.broadcasted_iota(
        jnp.int32, (rows, rows), 1
    )
    before = jnp.dot(
        tri.astype(F32).astype(BF16),
        chosen.astype(F32).astype(BF16),
        preferred_element_type=F32,
    )
    slot = jnp.where(chosen, before, jnp.float32(-1.0))

    for k in range(1, T):
        source = lax.rem(t + k, T)
        remote(
            conv_out.at[source], conv_in.at[source], a2a_send.at[source], a2a_recv.at[source], s, source
        ).wait_recv()
    total = jnp.zeros((rows, 1), F32)
    for j in range(T):
        total = total + jnp.sum(conv_in[j].astype(F32), axis=1, keepdims=True)
    average = total / (T * width)
    total = jnp.zeros((rows, 1), F32)
    for j in range(T):
        centered = conv_in[j].astype(F32) - average
        total = total + jnp.sum(centered * centered, axis=1, keepdims=True)
    scale = lax.rsqrt(total / (T * width) + epsilon)
    for j in range(T):
        cols = slice(j * width, (j + 1) * width)
        v = (conv_in[j].astype(F32) - average) * scale * gain_conv_ref[:, cols] + bias_conv_ref[
            :, cols
        ]
        act[j, :, :] = (v / (1.0 + jnp.exp(-v))).astype(BF16)

    for k in range(1, Z):
        from_z = lax.rem(z - k + Z, Z)
        row = 2 * from_z + core
        for j in range(1, S):
            source = lax.rem(s - j + S, S)
            remote(
                wfull.at[row, source],
                wfull.at[row, source],
                wx_send.at[j, from_z],
                wx_recv.at[source, from_z],
                source,
                t,
            ).wait_recv()
        c = remote(
            wfull.at[row], wfull.at[row], wp_send.at[from_z], wp_recv.at[from_z], s, partner
        )
        c.start()
        waits.append(c)
    loads[2].wait()
    for j in range(Z):
        row = 2 * j + 1 - core
        remote(wfull.at[row], wfull.at[row], wp_send.at[j], wp_recv.at[j], s, partner).wait_recv()

    def project(j, squares):
        cols = pl.ds(pl.multiple_of(j * piece, piece), piece)
        acc = residual[:, cols].astype(F32)
        part = jnp.zeros_like(acc)
        for i in range(T):
            part = part + jnp.dot(act[i], wfull[i, j], preferred_element_type=F32)
        state = (acc + part).astype(BF16)
        hidden[:, cols] = state
        state = state.astype(F32)
        return squares + jnp.sum(state * state, axis=1, keepdims=True)

    squares = lax.fori_loop(0, S, project, jnp.zeros((rows, 1), F32))
    scale = lax.rsqrt(squares / D + epsilon)

    def norm_cols(j, _):
        cols = pl.ds(pl.multiple_of(j * piece, piece), piece)
        normed[:, cols] = (hidden[:, cols].astype(F32) * scale * gain_moe_ref[:, cols]).astype(BF16)
        return 0

    lax.fori_loop(0, S, norm_cols, 0)

    slot_iota = lax.broadcasted_iota(jnp.int32, (rows, cap), 1).astype(F32)

    def column(array, expert):
        return jnp.sum(
            jnp.where(lane == expert + G, array, jnp.float32(0.0)), axis=1, keepdims=True
        )

    def gather_rows(expert, target):
        picks = (column(slot, expert) == slot_iota).astype(F32).astype(BF16)

        def cols_step(j, _):
            cols = pl.ds(pl.multiple_of(j * piece, piece), piece)
            target[:, cols] = lax.dot_general(
                picks,
                normed[:, cols],
                (((0,), (0,)), ((), ())),
                preferred_element_type=F32,
            ).astype(BF16)
            return 0

        lax.fori_loop(0, S, cols_step, 0)

    for k in range(1, S):
        expert = lax.rem(s + k, S)
        gather_rows(expert, outgoing.at[expert])
        remote(
            outgoing.at[expert], arrived.at[s], disp_send.at[expert], disp_recv.at[s], expert, t
        ).start()
    gather_rows(s, arrived.at[s])

    logits = jnp.dot(normed[...], router_ref[...], preferred_element_type=F32)
    exps = jnp.exp(logits)
    zero = jnp.float32(0.0)
    group_prob = jnp.sum(jnp.where(in_group, exps, zero), axis=1, keepdims=True) / jnp.sum(
        jnp.where(lane < G, exps, zero), axis=1, keepdims=True
    )
    chosen_exp = jnp.where(chosen, exps, zero)
    mix = group_prob * chosen_exp / jnp.sum(chosen_exp, axis=1, keepdims=True)

    for c in loads[3:]:
        c.wait()
    ff = gate_w.shape[2]
    ff_step = min(ff, 256)

    def expert_block(sender, target):
        def up_step(j, _):
            cols = pl.ds(pl.multiple_of(j * ff_step, ff_step), ff_step)
            x = arrived[sender]
            g = jnp.dot(x, gate_w[0, :, cols], preferred_element_type=F32)
            u = jnp.dot(x, up_w[0, :, cols], preferred_element_type=F32)
            ffn_hidden[:, cols] = (g / (1.0 + jnp.exp(-g)) * u).astype(BF16)
            return 0

        lax.fori_loop(0, ff // ff_step, up_step, 0)

        def down_step(j, _):
            cols = pl.ds(pl.multiple_of(j * piece, piece), piece)
            target[:, cols] = jnp.dot(
                ffn_hidden[...], down_w[0, :, cols], preferred_element_type=F32
            ).astype(BF16)
            return 0

        lax.fori_loop(0, S, down_step, 0)

    expert_block(s, returned.at[s])
    for k in range(1, S):
        sender = lax.rem(s - k + S, S)
        remote(
            outgoing.at[sender], arrived.at[sender], disp_send.at[sender], disp_recv.at[sender], sender, t
        ).wait_recv()
        expert_block(sender, results.at[sender])
        remote(
            results.at[sender], returned.at[s], ret_send.at[sender], ret_recv.at[s], sender, t
        ).start()

    for k in range(1, S):
        expert = lax.rem(s + k, S)
        remote(
            results.at[expert], returned.at[expert], ret_send.at[expert], ret_recv.at[expert], expert, t
        ).wait_recv()
    spreads = [
        jnp.where(column(slot, e) == slot_iota, column(mix, e), zero).astype(BF16)
        for e in range(E)
    ]

    def combine(j, _):
        cols = pl.ds(pl.multiple_of(j * piece, piece), piece)
        acc = jnp.zeros((rows, piece), F32)
        for e in range(E):
            acc = acc + jnp.dot(spreads[e], returned[e, :, cols], preferred_element_type=F32)
        out_ref[:, cols] = (hidden[:, cols].astype(F32) + acc).astype(BF16)
        return 0

    lax.fori_loop(0, S, combine, 0)

    for c in waits:
        c.wait_send()
    rim_done = None
    for k in range(1, T):
        to = lax.rem(t + k, T)
        remote(conv_out.at[to], conv_in.at[t], a2a_send.at[to], a2a_recv.at[t], s, to).wait_send()
    for k in range(1, S):
        to = lax.rem(s + k, S)
        remote(outgoing.at[to], arrived.at[s], disp_send.at[to], disp_recv.at[s], to, t).wait_send()
        remote(results.at[to], returned.at[s], ret_send.at[to], ret_recv.at[s], to, t).wait_send()


def body(
    S,
    T,
    conv_value,
    conv_gate,
    doc_ids,
    conv_kernel,
    norm_gain_conv,
    norm_bias_conv,
    proj_weight,
    residual,
    norm_gain_moe,
    group_router,
    expert_router,
    routing,
    expert_gate_w,
    expert_up_w,
    expert_down_w,
):
    tokens, width = conv_value.shape
    n_taps = conv_kernel.shape[0]
    rows, D = residual.shape
    wrows = proj_weight.shape[0]
    ff = expert_gate_w.shape[2]
    G = group_router.shape[1]
    E = expert_router.shape[1]
    cap = 2 * rows // E
    lanes = min(width, 128)
    start = jnp.sum((doc_ids[None, :] < doc_ids[:, None]).astype(jnp.int32), axis=1)
    position = jnp.arange(tokens, dtype=jnp.int32)
    least = jnp.where(start == 0, 0, n_taps - 1 - (position - start))
    least_tap = jnp.broadcast_to(least[:, None], (tokens, lanes))
    last_id = doc_ids[tokens - 1]
    rim_keep = jnp.broadcast_to(
        (doc_ids[tokens - HALO :] == last_id).astype(F32)[:, None], (HALO, width)
    )
    last_ids = jnp.full((16, width), last_id.astype(BF16))
    first_ids = jnp.full((16, width), doc_ids[0].astype(F32))
    router = jnp.concatenate(
        [group_router, expert_router, jnp.zeros((D, 128 - G - E), BF16)], axis=1
    )
    vmem = pl.BlockSpec(memory_space=pltpu.VMEM)
    hbm = pl.BlockSpec(memory_space=pl.ANY)
    dma = pltpu.SemaphoreType.DMA
    piece = D // S
    Z = T // 2
    return pl.pallas_call(
        functools.partial(kernel, S, T, G),
        out_shape=jax.ShapeDtypeStruct((rows, D), BF16),
        in_specs=[
            hbm, hbm, vmem, vmem, vmem, vmem, vmem, vmem, vmem, hbm, hbm, vmem, vmem, vmem,
            hbm, hbm, hbm,
        ],
        out_specs=vmem,
        scratch_shapes=[
            pltpu.VMEM((tokens, width), BF16),
            pltpu.VMEM((tokens, width), BF16),
            pltpu.VMEM((T, S, wrows, piece), BF16),
            pltpu.VMEM((rows, D), BF16),
            pltpu.VMEM((1, D, ff), BF16),
            pltpu.VMEM((1, D, ff), BF16),
            pltpu.VMEM((1, ff, D), BF16),
            pltpu.VMEM((HALO + 16, width), BF16),
            pltpu.VMEM((HALO + 16, width), BF16),
            pltpu.VMEM((tokens + HALO, width), F32),
            pltpu.VMEM((32, width), F32),
            pltpu.VMEM((T, rows, width), BF16),
            pltpu.VMEM((T, rows, width), BF16),
            pltpu.VMEM((T, rows, width), BF16),
            pltpu.VMEM((rows, D), BF16),
            pltpu.VMEM((rows, D), BF16),
            pltpu.VMEM((E, cap, D), BF16),
            pltpu.VMEM((E, cap, D), BF16),
            pltpu.VMEM((cap, ff), BF16),
            pltpu.VMEM((E, cap, D), BF16),
            pltpu.VMEM((E, cap, D), BF16),
            dma((6,)),
            dma((S,)),
            dma((2,)),
            dma((Z,)),
            dma((Z,)),
            dma((S, Z)),
            dma((S, Z)),
            dma((Z,)),
            dma((Z,)),
            dma((T,)),
            dma((T,)),
            dma((S,)),
            dma((S,)),
            dma((S,)),
            dma((S,)),
        ],
        compiler_params=pltpu.CompilerParams(
            collective_id=0, has_side_effects=True, vmem_limit_bytes=60 * 1024 * 1024
        ),
    )(
        conv_value,
        conv_gate,
        least_tap,
        rim_keep,
        last_ids,
        first_ids,
        conv_kernel,
        norm_gain_conv[None, :],
        norm_bias_conv[None, :],
        proj_weight,
        residual,
        norm_gain_moe[None, :],
        router,
        routing,
        expert_gate_w,
        expert_up_w,
        expert_down_w,
    )


def solution(mesh):
    placed = (
        P("sp", "tp"),
        P("sp", "tp"),
        P("sp"),
        P(None, "tp"),
        P(),
        P(),
        P("tp", None),
        P(("sp", "tp"), None),
        P(),
        P(),
        P(),
        P(("sp", "tp"), None),
        P("sp", None, None),
        P("sp", None, None),
        P("sp", None, None),
    )
    return jax.shard_map(
        functools.partial(body, mesh.shape["sp"], mesh.shape["tp"]),
        mesh=mesh,
        in_specs=placed,
        out_specs=P(("sp", "tp"), None),
        check_vma=False,
    )
```

```python
import functools

import jax
import jax.numpy as jnp
from jax import lax
from jax.experimental import pallas as pl
from jax.experimental.pallas import tpu as pltpu
from jax.sharding import PartitionSpec as P

epsilon = 1e-06
MESH = pl.DeviceIdType.MESH
F32 = jnp.float32
BF16 = jnp.bfloat16
HALO = 32


def gate(value, gate_value):
    return (value.astype(F32) * jax.nn.sigmoid(gate_value.astype(F32))).astype(BF16)


def kernel(
    S,
    T,
    G,
    value_hbm,
    gate_hbm,
    least_tap_ref,
    ids_ref,
    kernel_ref,
    gain_conv_ref,
    bias_conv_ref,
    weight_hbm,
    residual_hbm,
    gain_moe_ref,
    group_router_ref,
    expert_router_ref,
    routing_ref,
    gate_w_hbm,
    up_w_hbm,
    down_w_hbm,
    out_ref,
    value,
    gates,
    wfull,
    residual,
    gate_w,
    up_w,
    down_w,
    rim_out,
    rim_in,
    padded,
    taps,
    conv_out,
    conv_in,
    act,
    hidden,
    normed,
    outgoing,
    arrived,
    ffn_hidden,
    results,
    returned,
    local_sem,
    wl_sem,
    rim_sem,
    wz_send,
    wz_recv,
    wx_send,
    wx_recv,
    wp_send,
    wp_recv,
    a2a_send,
    a2a_recv,
    disp_send,
    disp_recv,
    ret_send,
    ret_recv,
):
    s = lax.axis_index("sp")
    t = lax.axis_index("tp")
    Z = T // 2
    z = t // 2
    core = t % 2
    partner = 2 * z + 1 - core
    tokens, width = value.shape
    block = tokens // T
    n_taps = kernel_ref.shape[0]
    piece = wfull.shape[3]
    D = S * piece

    def remote(src, dst, send, recv, sp_to, tp_to):
        return pltpu.make_async_remote_copy(
            src_ref=src,
            dst_ref=dst,
            send_sem=send,
            recv_sem=recv,
            device_id=(sp_to, tp_to),
            device_id_type=MESH,
        )

    loads = [
        pltpu.make_async_copy(a, b, local_sem.at[i])
        for i, (a, b) in enumerate(
            [
                (value_hbm, value),
                (gate_hbm, gates),
                (residual_hbm, residual),
                (gate_w_hbm, gate_w),
                (up_w_hbm, up_w),
                (down_w_hbm, down_w),
            ]
        )
    ]
    own_w = [
        pltpu.make_async_copy(
            weight_hbm.at[:, pl.ds(j * piece, piece)], wfull.at[t, j], wl_sem.at[j]
        )
        for j in range(S)
    ]
    loads[0].start()
    loads[1].start()
    for c in own_w:
        c.start()
    for c in loads[2:]:
        c.start()

    barrier = pltpu.get_barrier_semaphore()
    for k in range(1, T):
        pl.semaphore_signal(
            barrier, inc=1, device_id=(s, lax.rem(t + k, T)), device_id_type=MESH
        )
    for k in range(1, S):
        pl.semaphore_signal(
            barrier, inc=1, device_id=(lax.rem(s + k, S), t), device_id_type=MESH
        )
    pl.semaphore_wait(barrier, T + S - 2)

    for c in own_w:
        c.wait()
    waits = []
    for k in range(1, Z):
        to = 2 * lax.rem(z + k, Z) + core
        c = remote(wfull.at[t, s], wfull.at[t, s], wz_send.at[k], wz_recv.at[z], s, to)
        c.start()
        waits.append(c)
    c = remote(wfull.at[t], wfull.at[t], wp_send.at[z], wp_recv.at[z], s, partner)
    c.start()
    waits.append(c)

    loads[0].wait()
    loads[1].wait()
    tail = pl.ds(tokens - HALO, HALO)
    last_reach = jnp.max(least_tap_ref[tokens - 1 : tokens, :], axis=1, keepdims=True)
    newer = lax.broadcasted_iota(jnp.int32, (HALO, width), 0) >= last_reach + HALO - n_taps
    rim = jnp.where(newer, gate(value[tail, :], gates[tail, :]).astype(F32), jnp.float32(0.0))
    rim_out[0:HALO, :] = rim.astype(BF16)
    rim_out[HALO : HALO + 16, :] = jnp.full(
        (16, width), ids_ref[tokens - 1].astype(F32), F32
    ).astype(BF16)
    rim_copy = remote(
        rim_out, rim_in, rim_sem.at[0], rim_sem.at[1], lax.rem(s + 1, S), t
    )
    rim_copy.start()

    def gate_rows(i, _):
        rows = pl.ds(pl.multiple_of(i * 64, 64), 64)
        to_rows = pl.ds(pl.multiple_of(HALO + i * 64, 32), 64)
        padded[to_rows, :] = gate(value[rows, :], gates[rows, :]).astype(F32)
        return 0

    lax.fori_loop(0, tokens // 64, gate_rows, 0)
    taps[0:n_taps, :] = kernel_ref[...].astype(F32)
    rim_copy.wait()
    same = (rim_in[HALO : HALO + 1, :].astype(F32) == ids_ref[0].astype(F32)) & (s > 0)
    padded[0:HALO, :] = jnp.where(same, rim_in[0:HALO, :].astype(F32), jnp.float32(0.0))

    step_rows = 32 if block % 32 == 0 else 8
    lanes = min(width, 128)

    def conv_block(owner):
        def conv_rows(i, _):
            base = pl.multiple_of(owner * block + i * step_rows, 8)
            least = least_tap_ref[pl.ds(base, step_rows), :]
            window = padded[pl.ds(base, step_rows + HALO), :]
            total = jnp.zeros((step_rows, width), F32)
            for tap in range(n_taps):
                at = tap + HALO + 1 - n_taps
                valid = least <= tap
                product = window[at : at + step_rows, :] * taps[tap : tap + 1, :]
                parts = [
                    jnp.where(valid, product[:, j : j + lanes], jnp.float32(0.0))
                    for j in range(0, width, lanes)
                ]
                total = total + jnp.concatenate(parts, axis=1)
            conv_out[
                owner, pl.ds(pl.multiple_of(i * step_rows, step_rows), step_rows), :
            ] = total.astype(BF16)
            return 0

        lax.fori_loop(0, block // step_rows, conv_rows, 0)

    def conv_send(k, _):
        owner = lax.rem(t + k, T)
        conv_block(owner)
        remote(
            conv_out.at[owner],
            conv_in.at[t],
            a2a_send.at[owner],
            a2a_recv.at[t],
            s,
            owner,
        ).start()
        return 0

    done = 1
    for k in range(1, Z):
        upto = T - 2 * (Z - 1 - k)
        lax.fori_loop(done, upto, conv_send, 0)
        done = upto
        from_z = lax.rem(z - k + Z, Z)
        row = 2 * from_z + core
        remote(
            wfull.at[row, s], wfull.at[row, s], wz_send.at[k], wz_recv.at[from_z], s, t
        ).wait_recv()
        for j in range(1, S):
            c = remote(
                wfull.at[row, s],
                wfull.at[row, s],
                wx_send.at[j, from_z],
                wx_recv.at[s, from_z],
                lax.rem(s + j, S),
                t,
            )
            c.start()
            waits.append(c)
    conv_block(t)
    conv_in[t, :, :] = conv_out[t, :, :]

    rows = block
    E = S
    cap = 2 * rows // E
    lane = lax.broadcasted_iota(jnp.int32, (rows, 128), 1)
    eye = lax.broadcasted_iota(jnp.int32, (rows, rows), 0) == lax.broadcasted_iota(
        jnp.int32, (rows, rows), 1
    )
    named = lax.dot_general(
        eye.astype(F32).astype(BF16),
        routing_ref[...].astype(F32).astype(BF16),
        (((1,), (1,)), ((), ())),
        preferred_element_type=F32,
    )
    first = named[:, 0:1]
    second = named[:, 1:2]
    lane_f = lane.astype(F32)
    chosen = (lane_f == first) | (lane_f == second)
    per_group = E // G
    group_low = lane_f * per_group
    in_group = (first >= group_low) & (first < group_low + per_group)
    tri = lax.broadcasted_iota(jnp.int32, (rows, rows), 0) > lax.broadcasted_iota(
        jnp.int32, (rows, rows), 1
    )
    before = jnp.dot(
        tri.astype(F32).astype(BF16),
        chosen.astype(F32).astype(BF16),
        preferred_element_type=F32,
    )
    slot = jnp.where(chosen, before, jnp.float32(-1.0))

    for k in range(1, T):
        source = lax.rem(t + k, T)
        remote(
            conv_out.at[source], conv_in.at[source], a2a_send.at[source], a2a_recv.at[source], s, source
        ).wait_recv()
    total = jnp.zeros((rows, 1), F32)
    for j in range(T):
        total = total + jnp.sum(conv_in[j].astype(F32), axis=1, keepdims=True)
    average = total / (T * width)
    total = jnp.zeros((rows, 1), F32)
    for j in range(T):
        centered = conv_in[j].astype(F32) - average
        total = total + jnp.sum(centered * centered, axis=1, keepdims=True)
    scale = lax.rsqrt(total / (T * width) + epsilon)
    for j in range(T):
        cols = slice(j * width, (j + 1) * width)
        v = (conv_in[j].astype(F32) - average) * scale * gain_conv_ref[:, cols] + bias_conv_ref[
            :, cols
        ]
        act[j, :, :] = (v / (1.0 + jnp.exp(-v))).astype(BF16)

    for k in range(1, Z):
        from_z = lax.rem(z - k + Z, Z)
        row = 2 * from_z + core
        for j in range(1, S):
            source = lax.rem(s - j + S, S)
            remote(
                wfull.at[row, source],
                wfull.at[row, source],
                wx_send.at[j, from_z],
                wx_recv.at[source, from_z],
                source,
                t,
            ).wait_recv()
        c = remote(
            wfull.at[row], wfull.at[row], wp_send.at[from_z], wp_recv.at[from_z], s, partner
        )
        c.start()
        waits.append(c)
    loads[2].wait()
    for j in range(Z):
        row = 2 * j + 1 - core
        remote(wfull.at[row], wfull.at[row], wp_send.at[j], wp_recv.at[j], s, partner).wait_recv()

    def project(j, squares):
        cols = pl.ds(pl.multiple_of(j * piece, piece), piece)
        acc = residual[:, cols].astype(F32)
        part = jnp.zeros_like(acc)
        for i in range(T):
            part = part + jnp.dot(act[i], wfull[i, j], preferred_element_type=F32)
        state = (acc + part).astype(BF16)
        hidden[:, cols] = state
        state = state.astype(F32)
        return squares + jnp.sum(state * state, axis=1, keepdims=True)

    squares = lax.fori_loop(0, S, project, jnp.zeros((rows, 1), F32))
    scale = lax.rsqrt(squares / D + epsilon)

    def norm_cols(j, _):
        cols = pl.ds(pl.multiple_of(j * piece, piece), piece)
        normed[:, cols] = (hidden[:, cols].astype(F32) * scale * gain_moe_ref[:, cols]).astype(BF16)
        return 0

    lax.fori_loop(0, S, norm_cols, 0)

    slot_iota = lax.broadcasted_iota(jnp.int32, (rows, cap), 1).astype(F32)

    def column(array, expert):
        mine = lane[:, : array.shape[1]] == expert
        return jnp.sum(jnp.where(mine, array, jnp.float32(0.0)), axis=1, keepdims=True)

    def gather_rows(expert, target):
        picks = (column(slot, expert) == slot_iota).astype(F32).astype(BF16)

        def cols_step(j, _):
            cols = pl.ds(pl.multiple_of(j * piece, piece), piece)
            target[:, cols] = lax.dot_general(
                picks,
                normed[:, cols],
                (((0,), (0,)), ((), ())),
                preferred_element_type=F32,
            ).astype(BF16)
            return 0

        lax.fori_loop(0, S, cols_step, 0)

    for k in range(1, S):
        expert = lax.rem(s + k, S)
        gather_rows(expert, outgoing.at[expert])
        remote(
            outgoing.at[expert], arrived.at[s], disp_send.at[expert], disp_recv.at[s], expert, t
        ).start()
    gather_rows(s, arrived.at[s])

    def logits(router):
        return lax.dot_general(
            normed[...], router[...], (((1,), (1,)), ((), ())), preferred_element_type=F32
        )

    group_exp = jnp.exp(logits(group_router_ref))
    expert_exp = jnp.exp(logits(expert_router_ref))
    zero = jnp.float32(0.0)
    group_prob = jnp.sum(
        jnp.where(in_group[:, :G], group_exp, zero), axis=1, keepdims=True
    ) / jnp.sum(group_exp, axis=1, keepdims=True)
    chosen_exp = jnp.where(chosen[:, :E], expert_exp, zero)
    mix = group_prob * chosen_exp / jnp.sum(chosen_exp, axis=1, keepdims=True)

    for c in loads[3:]:
        c.wait()
    ff = gate_w.shape[2]
    ff_step = min(ff, 256)

    def expert_block(sender, target):
        def up_step(j, _):
            cols = pl.ds(pl.multiple_of(j * ff_step, ff_step), ff_step)
            x = arrived[sender]
            g = jnp.dot(x, gate_w[0, :, cols], preferred_element_type=F32)
            u = jnp.dot(x, up_w[0, :, cols], preferred_element_type=F32)
            ffn_hidden[:, cols] = (g / (1.0 + jnp.exp(-g)) * u).astype(BF16)
            return 0

        lax.fori_loop(0, ff // ff_step, up_step, 0)

        def down_step(j, _):
            cols = pl.ds(pl.multiple_of(j * piece, piece), piece)
            target[:, cols] = jnp.dot(
                ffn_hidden[...], down_w[0, :, cols], preferred_element_type=F32
            ).astype(BF16)
            return 0

        lax.fori_loop(0, S, down_step, 0)

    expert_block(s, returned.at[s])
    for k in range(1, S):
        sender = lax.rem(s - k + S, S)
        remote(
            outgoing.at[sender], arrived.at[sender], disp_send.at[sender], disp_recv.at[sender], sender, t
        ).wait_recv()
        expert_block(sender, results.at[sender])
        remote(
            results.at[sender], returned.at[s], ret_send.at[sender], ret_recv.at[s], sender, t
        ).start()

    for k in range(1, S):
        expert = lax.rem(s + k, S)
        remote(
            results.at[expert], returned.at[expert], ret_send.at[expert], ret_recv.at[expert], expert, t
        ).wait_recv()
    spreads = [
        jnp.where(column(slot, e) == slot_iota, column(mix, e), zero).astype(BF16)
        for e in range(E)
    ]

    def combine(j, _):
        cols = pl.ds(pl.multiple_of(j * piece, piece), piece)
        acc = jnp.zeros((rows, piece), F32)
        for e in range(E):
            acc = acc + jnp.dot(spreads[e], returned[e, :, cols], preferred_element_type=F32)
        out_ref[:, cols] = (hidden[:, cols].astype(F32) + acc).astype(BF16)
        return 0

    lax.fori_loop(0, S, combine, 0)

    for c in waits:
        c.wait_send()
    for k in range(1, T):
        to = lax.rem(t + k, T)
        remote(conv_out.at[to], conv_in.at[t], a2a_send.at[to], a2a_recv.at[t], s, to).wait_send()
    for k in range(1, S):
        to = lax.rem(s + k, S)
        remote(outgoing.at[to], arrived.at[s], disp_send.at[to], disp_recv.at[s], to, t).wait_send()
        remote(results.at[to], returned.at[s], ret_send.at[to], ret_recv.at[s], to, t).wait_send()


def body(
    S,
    T,
    conv_value,
    conv_gate,
    doc_ids,
    conv_kernel,
    norm_gain_conv,
    norm_bias_conv,
    proj_weight,
    residual,
    norm_gain_moe,
    group_router,
    expert_router,
    routing,
    expert_gate_w,
    expert_up_w,
    expert_down_w,
):
    tokens, width = conv_value.shape
    n_taps = conv_kernel.shape[0]
    rows, D = residual.shape
    wrows = proj_weight.shape[0]
    ff = expert_gate_w.shape[2]
    G = group_router.shape[1]
    E = expert_router.shape[1]
    cap = 2 * rows // E
    lanes = min(width, 128)
    start = jnp.sum((doc_ids[None, :] < doc_ids[:, None]).astype(jnp.int32), axis=1)
    position = jnp.arange(tokens, dtype=jnp.int32)
    least = jnp.where(start == 0, 0, n_taps - 1 - (position - start))
    least_tap = jnp.broadcast_to(least[:, None], (tokens, lanes))
    vmem = pl.BlockSpec(memory_space=pltpu.VMEM)
    hbm = pl.BlockSpec(memory_space=pl.ANY)
    smem = pl.BlockSpec(memory_space=pltpu.SMEM)
    dma = pltpu.SemaphoreType.DMA
    piece = D // S
    Z = T // 2
    return pl.pallas_call(
        functools.partial(kernel, S, T, G),
        out_shape=jax.ShapeDtypeStruct((rows, D), BF16),
        in_specs=[
            hbm, hbm, vmem, smem, vmem, vmem, vmem, hbm, hbm, vmem, vmem, vmem, vmem,
            hbm, hbm, hbm,
        ],
        out_specs=vmem,
        scratch_shapes=[
            pltpu.VMEM((tokens, width), BF16),
            pltpu.VMEM((tokens, width), BF16),
            pltpu.VMEM((T, S, wrows, piece), BF16),
            pltpu.VMEM((rows, D), BF16),
            pltpu.VMEM((1, D, ff), BF16),
            pltpu.VMEM((1, D, ff), BF16),
            pltpu.VMEM((1, ff, D), BF16),
            pltpu.VMEM((HALO + 16, width), BF16),
            pltpu.VMEM((HALO + 16, width), BF16),
            pltpu.VMEM((tokens + HALO, width), F32),
            pltpu.VMEM((32, width), F32),
            pltpu.VMEM((T, rows, width), BF16),
            pltpu.VMEM((T, rows, width), BF16),
            pltpu.VMEM((T, rows, width), BF16),
            pltpu.VMEM((rows, D), BF16),
            pltpu.VMEM((rows, D), BF16),
            pltpu.VMEM((E, cap, D), BF16),
            pltpu.VMEM((E, cap, D), BF16),
            pltpu.VMEM((cap, ff), BF16),
            pltpu.VMEM((E, cap, D), BF16),
            pltpu.VMEM((E, cap, D), BF16),
            dma((6,)),
            dma((S,)),
            dma((2,)),
            dma((Z,)),
            dma((Z,)),
            dma((S, Z)),
            dma((S, Z)),
            dma((Z,)),
            dma((Z,)),
            dma((T,)),
            dma((T,)),
            dma((S,)),
            dma((S,)),
            dma((S,)),
            dma((S,)),
        ],
        compiler_params=pltpu.CompilerParams(
            collective_id=0, has_side_effects=True, vmem_limit_bytes=60 * 1024 * 1024
        ),
    )(
        conv_value,
        conv_gate,
        least_tap,
        doc_ids,
        conv_kernel,
        norm_gain_conv[None, :],
        norm_bias_conv[None, :],
        proj_weight,
        residual,
        norm_gain_moe[None, :],
        group_router.T,
        expert_router.T,
        routing.T,
        expert_gate_w,
        expert_up_w,
        expert_down_w,
    )


def solution(mesh):
    placed = (
        P("sp", "tp"),
        P("sp", "tp"),
        P("sp"),
        P(None, "tp"),
        P(),
        P(),
        P("tp", None),
        P(("sp", "tp"), None),
        P(),
        P(),
        P(),
        P(("sp", "tp"), None),
        P("sp", None, None),
        P("sp", None, None),
        P("sp", None, None),
    )
    return jax.shard_map(
        functools.partial(body, mesh.shape["sp"], mesh.shape["tp"]),
        mesh=mesh,
        in_specs=placed,
        out_specs=P(("sp", "tp"), None),
        check_vma=False,
    )
```
